512 devices in a mesh: tp: 16 (over y, x), dp: 32 (over z, core).
Axes of the slice: x: 4, y: 4, z: 16, core: 2. Of those that a mesh axis runs over, the one named last changes fastest.
Arguments:
- tokens: bfloat16 [64, 4096], P('tp', 'dp'), may hold values from -12.5 to 12.5
- gain_first: bfloat16 [4096], P('dp'), may hold values from 0.099609375 to 1.8984375
- query_first: bfloat16 [4096, 2048], P('dp', 'tp'), may hold values from -0.09375 to 0.09375
- key_first: bfloat16 [4096, 2048], P('dp', 'tp'), may hold values from -0.09375 to 0.09375
- value_first: bfloat16 [4096, 4096], P('dp', 'tp'), may hold values from -0.09375 to 0.09375
- outgate_first: bfloat16 [4096, 4096], P('dp', 'tp'), may hold values from -0.09375 to 0.09375
- inputgate_first: bfloat16 [4096, 16], P('dp'), may hold values from -0.09375 to 0.09375
- forget_first: bfloat16 [4096, 16], P('dp'), may hold values from -0.09375 to 0.09375
- mixing_first: bfloat16 [4096, 4096], P('tp', 'dp'), may hold values from -0.09375 to 0.09375
- cell_first: float32 [64, 16, 256, 128], P('dp', 'tp'), may hold values from -6 to 6
- norm_first: float32 [64, 16, 128], P('dp', 'tp'), may hold values from -6 to 6
- stabilizer_first: float32 [64, 16], P('dp', 'tp'), may hold values from -3 to 115
- gain_second: bfloat16 [4096], P('dp'), may hold values from 0.099609375 to 1.8984375
- query_second: bfloat16 [4096, 2048], P('dp', 'tp'), may hold values from -0.09375 to 0.09375
- key_second: bfloat16 [4096, 2048], P('dp', 'tp'), may hold values from -0.09375 to 0.09375
- value_second: bfloat16 [4096, 4096], P('dp', 'tp'), may hold values from -0.09375 to 0.09375
- outgate_second: bfloat16 [4096, 4096], P('dp', 'tp'), may hold values from -0.09375 to 0.09375
- inputgate_second: bfloat16 [4096, 16], P('dp'), may hold values from -0.09375 to 0.09375
- forget_second: bfloat16 [4096, 16], P('dp'), may hold values from -0.09375 to 0.09375
- mixing_second: bfloat16 [4096, 4096], P('tp', 'dp'), may hold values from -0.09375 to 0.09375
- cell_second: float32 [64, 16, 256, 128], P('dp', 'tp'), may hold values from -6 to 6
- norm_second: float32 [64, 16, 128], P('dp', 'tp'), may hold values from -6 to 6
- stabilizer_second: float32 [64, 16], P('dp', 'tp'), may hold values from -3 to 115
Outputs:
- hidden: bfloat16 [64, 4096], P('tp', 'dp')
- cell_first_next: float32 [64, 16, 256, 128], P('dp', 'tp')
- norm_first_next: float32 [64, 16, 128], P('dp', 'tp')
- stabilizer_first_next: float32 [64, 16], P('dp', 'tp')
- cell_second_next: float32 [64, 16, 256, 128], P('dp', 'tp')
- norm_second_next: float32 [64, 16, 128], P('dp', 'tp')
- stabilizer_second_next: float32 [64, 16], P('dp', 'tp')
The draws below stay inside these ranges and needn't reach their ends.
All inputs are finite; a program needn't handle non-finite values.
Results may differ from the reference program's by a relative error of at most 0.023.
Values may be sent and summed in bfloat16 or wider, within the bound.
A program may use at most 64 MiB of HBM per device.

```python
import jax
import jax.numpy as jnp
from jax import lax

D = 4096
HEADS = 16
DHK = 128
DHV = 256
BATCH = 64


def stabilizer_law(key):
    first_key = jax.random.fold_in(key, 0)
    base = jax.random.uniform(first_key, (BATCH, HEADS), jnp.float32, -3.0, 3.0)
    return base


def draw_stabilizer_first(key, part):
    return stabilizer_law(jax.random.fold_in(key, 1))


def draw_stabilizer_second(key, part):
    return stabilizer_law(jax.random.fold_in(key, 2))


def draw_tokens(key, part):
    own_key = jax.random.fold_in(key, 5)
    first_key = jax.random.fold_in(own_key, 0)
    noise = jnp.clip(jax.random.normal(first_key, (BATCH, D), jnp.float32), -4.0, 4.0)
    ramp = jnp.exp(jnp.linspace(-0.7, 0.7, D, dtype=jnp.float32))
    return (noise * ramp[None, :]).astype(jnp.bfloat16)


def block_scale(rng, shape, cuts, low, top_value):
    level = 1.0
    for dim, blocks in cuts:
        heights = jax.random.uniform(jax.random.fold_in(jax.random.fold_in(rng, 6), dim), (blocks,), jnp.float32, low / len(cuts), top_value / len(cuts))
        level = level * jnp.repeat(jnp.exp(heights), shape[dim] // blocks).reshape((-1,) + (1,) * (len(shape) - 1 - dim))
    return level


def gaussian(key, dims, width, most, shards=(), kind=jnp.bfloat16):
    array = width * jax.random.normal(key, dims, jnp.float32)
    if shards:
        array = array * block_scale(key, dims, shards, -0.22, 0.18)
    return jnp.clip(array, -most, most).astype(kind)


def setup_inputs(seed: int = 0) -> dict:
    splits = jax.random.split(jax.random.key(seed), 24)
    return {
        "tokens": draw_tokens(jax.random.fold_in(splits[23], 71), 0),
        "gain_first": jnp.clip(1.0 + 0.18 * jax.random.normal(splits[1], (D,), jnp.float32), 0.099609375, 1.8984375).astype(jnp.bfloat16),
        "query_first": gaussian(splits[2], (D, HEADS * DHK), D ** -0.5, 0.09375, ((0, 32), (1, 16))),
        "key_first": gaussian(splits[3], (D, HEADS * DHK), D ** -0.5, 0.09375, ((0, 32), (1, 16))),
        "value_first": gaussian(splits[4], (D, HEADS * DHV), D ** -0.5, 0.09375, ((0, 32), (1, 16))),
        "outgate_first": gaussian(splits[5], (D, HEADS * DHV), D ** -0.5, 0.09375, ((0, 32), (1, 16))),
        "inputgate_first": gaussian(splits[6], (D, HEADS), D ** -0.5, 0.09375, ((0, 32),)),
        "forget_first": gaussian(splits[7], (D, HEADS), D ** -0.5, 0.09375, ((0, 32),)),
        "mixing_first": gaussian(splits[8], (HEADS * DHV, D), (HEADS * DHV) ** -0.5, 0.09375, ((0, 16), (1, 32))),
        "cell_first": gaussian(splits[9], (BATCH, HEADS, DHV, DHK), 1.0, 6.0, ((0, 32), (1, 16)), jnp.float32),
        "norm_first": gaussian(splits[10], (BATCH, HEADS, DHK), 1.0, 6.0, ((0, 32), (1, 16)), jnp.float32),
        "stabilizer_first": draw_stabilizer_first(jax.random.fold_in(splits[23], 71), 0),
        "gain_second": jnp.clip(1.0 + 0.18 * jax.random.normal(splits[12], (D,), jnp.float32), 0.099609375, 1.8984375).astype(jnp.bfloat16),
        "query_second": gaussian(splits[13], (D, HEADS * DHK), D ** -0.5, 0.09375, ((0, 32), (1, 16))),
        "key_second": gaussian(splits[14], (D, HEADS * DHK), D ** -0.5, 0.09375, ((0, 32), (1, 16))),
        "value_second": gaussian(splits[15], (D, HEADS * DHV), D ** -0.5, 0.09375, ((0, 32), (1, 16))),
        "outgate_second": gaussian(splits[16], (D, HEADS * DHV), D ** -0.5, 0.09375, ((0, 32), (1, 16))),
        "inputgate_second": gaussian(splits[17], (D, HEADS), D ** -0.5, 0.09375, ((0, 32),)),
        "forget_second": gaussian(splits[18], (D, HEADS), D ** -0.5, 0.09375, ((0, 32),)),
        "mixing_second": gaussian(splits[19], (HEADS * DHV, D), (HEADS * DHV) ** -0.5, 0.09375, ((0, 16), (1, 32))),
        "cell_second": gaussian(splits[20], (BATCH, HEADS, DHV, DHK), 1.0, 6.0, ((0, 32), (1, 16)), jnp.float32),
        "norm_second": gaussian(splits[21], (BATCH, HEADS, DHK), 1.0, 6.0, ((0, 32), (1, 16)), jnp.float32),
        "stabilizer_second": draw_stabilizer_second(jax.random.fold_in(splits[23], 71), 0),
    }


eps = 1e-06

def cell_step(stream, gain, w_query, w_key, w_value, w_outgate, w_input, w_forget, w_mixing, cell_state, norm_state, stabilizer):
    batch_rows = stream.shape[0]
    widened = stream.astype(jnp.float32)
    squares = lax.optimization_barrier(jnp.sum(widened * widened, axis=1))
    row_scale = lax.rsqrt(squares / D + eps)[:, None]
    scaled = (widened * gain.astype(jnp.float32)).astype(jnp.bfloat16)

    def project(weight):
        return jnp.dot(scaled, weight, preferred_element_type=jnp.float32) * row_scale
    queries = project(w_query).reshape(batch_rows, HEADS, DHK) * DHK ** (-0.5)
    key_rows = project(w_key).reshape(batch_rows, HEADS, DHK)
    value_rows = project(w_value).reshape(batch_rows, HEADS, DHV)
    outgate_pre = project(w_outgate)
    input_pre = project(w_input)
    forget_pre = project(w_forget)
    log_forget = jax.nn.log_sigmoid(forget_pre)
    stab_next = jnp.maximum(log_forget + stabilizer, input_pre)
    retain = jnp.exp(log_forget + stabilizer - stab_next)
    admitted = jnp.exp(input_pre - stab_next)
    cell_next = retain[:, :, None, None] * cell_state + admitted[:, :, None, None] * value_rows[:, :, :, None] * key_rows[:, :, None, :]
    norm_next = retain[:, :, None] * norm_state + admitted[:, :, None] * key_rows
    numerator = jnp.einsum('shvd,shd->shv', cell_next, queries, precision=lax.Precision.HIGHEST)
    denominator = jnp.einsum('shd,shd->sh', norm_next, queries, precision=lax.Precision.HIGHEST)
    readout = numerator / jnp.maximum(jnp.abs(denominator), 1.0)[:, :, None]
    gated_rows = (readout.reshape(batch_rows, HEADS * DHV) * jax.nn.sigmoid(outgate_pre)).astype(jnp.bfloat16)
    result = (widened + jnp.dot(gated_rows, w_mixing, preferred_element_type=jnp.float32)).astype(jnp.bfloat16)
    return (result, cell_next, norm_next, stab_next)

def reference(tokens, gain_first, query_first, key_first, value_first, outgate_first, inputgate_first, forget_first, mixing_first, cell_first, norm_first, stabilizer_first, gain_second, query_second, key_second, value_second, outgate_second, inputgate_second, forget_second, mixing_second, cell_second, norm_second, stabilizer_second):
    middle, cell_one, norm_one, stab_one = cell_step(tokens, gain_first, query_first, key_first, value_first, outgate_first, inputgate_first, forget_first, mixing_first, cell_first, norm_first, stabilizer_first)
    hidden, cell_two, norm_two, stab_two = cell_step(middle, gain_second, query_second, key_second, value_second, outgate_second, inputgate_second, forget_second, mixing_second, cell_second, norm_second, stabilizer_second)
    return (hidden, cell_one, norm_one, stab_one, cell_two, norm_two, stab_two)
```

```python
import functools

import jax
import jax.numpy as jnp
from jax import lax
from jax.experimental import pallas as pl
from jax.experimental.pallas import tpu as pltpu
from jax.sharding import PartitionSpec as P

DHK = 128
DHV = 256
EPS = 1e-06
ROWS = 16
MESH = pl.DeviceIdType.MESH
F32 = jnp.float32
BF16 = jnp.bfloat16


def kernel(T, N, *refs):
    (x_in, *rest) = refs
    ins = (rest[:11], rest[11:22])
    outs = rest[22:29]
    (
        wcat,
        wmix,
        wif,
        wif_own,
        gains,
        cell,
        norm,
        stab,
        cellt_hi,
        cellt_lo,
        xg,
        xs,
        stage,
        sbuf,
        rbuf,
        gbuf,
        gs,
        ybuf,
        ysc,
        ysend,
        yrecv,
        load_sems,
        out_sems,
        send_sems,
        recv_sems,
    ) = rest[29:]
    t = lax.axis_index("tp")
    d = lax.axis_index("dp")
    features = DHK * N

    def tp_peer(o):
        return {"tp": lax.rem(t + o, T)}

    def dp_peer(o):
        return {"dp": lax.rem(d + o, N)}

    far_dp = sorted(range(1, N), key=lambda o: abs(o - N // 2))

    x_load = pltpu.make_async_copy(x_in, xg.at[t], load_sems.at[0])
    x_load.start()
    loads = []
    for c in range(2):
        gain, wq, wk, wv, wo, wi, wf, wm, state, nstate, mstate = ins[c]
        pairs = [
            (gain, gains.at[c]),
            (wq, wcat.at[c, :, 0:128]),
            (wk, wcat.at[c, :, 128:256]),
            (wv, wcat.at[c, :, 256:512]),
            (wo, wcat.at[c, :, 512:768]),
            (wi, wif.at[c, 0]),
            (wf, wif.at[c, 1]),
            (state, cell.at[c]),
            (nstate, norm.at[c]),
            (mstate, stab.at[c]),
            (wm, wmix.at[c]),
        ]
        group = []
        for n, (src, dst) in enumerate(pairs):
            copy = pltpu.make_async_copy(src, dst, load_sems.at[1 + 11 * c + n])
            copy.start()
            group.append(copy)
        loads.append(group)

    barrier = pltpu.get_barrier_semaphore()
    for o in far_dp:
        pl.semaphore_signal(barrier, inc=1, device_id=dp_peer(o), device_id_type=MESH)
    for o in range(1, T):
        pl.semaphore_signal(barrier, inc=1, device_id=tp_peer(o), device_id_type=MESH)

    def prepare(c):
        mine = lax.broadcasted_iota(jnp.int32, (T, DHK), 0) == t
        for g in range(2):
            wif_own[c, g] = jnp.sum(jnp.where(mine, wif[c, g].astype(F32), 0.0), axis=0, keepdims=True)
        for s in range(2):
            old = cell[c, s * DHV : (s + 1) * DHV, :]
            turned = old.T
            high = turned.astype(BF16)
            cellt_hi[c, :, s * DHV : (s + 1) * DHV] = high
            cellt_lo[c, :, s * DHV : (s + 1) * DHV] = (turned - high.astype(F32)).astype(BF16)

    for copy in loads[0]:
        copy.wait()
    prepare(0)

    pl.semaphore_wait(barrier, T + N - 2)

    x_load.wait()
    sends = []

    def send(src, dst, phase, peer):
        copy = pltpu.make_async_remote_copy(
            src_ref=src,
            dst_ref=dst,
            send_sem=send_sems.at[phase],
            recv_sem=recv_sems.at[phase],
            device_id=peer,
            device_id_type=MESH,
        )
        copy.start()
        return copy

    def wait_recv(ref, phase):
        pltpu.make_async_copy(ref, ref, recv_sems.at[phase]).wait()

    def wait_send(ref, phase):
        pltpu.make_async_copy(ref, ref, send_sems.at[phase]).wait()

    for o in range(1, T):
        send(xg.at[t], xg.at[t], 0, tp_peer(o))
    sends.append((xg.at[pl.ds(0, T - 1)], 0))

    for copy in loads[1]:
        copy.wait()
    prepare(1)

    wait_recv(xg.at[pl.ds(0, T - 1)], 0)
    for j in range(T):
        xs[4 * j : 4 * j + 4, :] = xg[j].astype(F32)

    def project(c, phase):
        wide = jnp.concatenate([xs[pl.ds(0, N, stride=2), :], xs[pl.ds(1, N, stride=2), :]], axis=0)
        scaled = (wide * gains[c].astype(F32)).astype(BF16)
        squares = jnp.sum(wide * wide, axis=1, keepdims=True)
        scaled_wide = scaled.astype(F32)
        wi_row = wif_own[c, 0]
        wf_row = wif_own[c, 1]
        i_part = jnp.sum(scaled_wide * wi_row, axis=1, keepdims=True)
        f_part = jnp.sum(scaled_wide * wf_row, axis=1, keepdims=True)
        lane = lax.broadcasted_iota(jnp.int32, (2 * N, 128), 1)
        misc = jnp.where(lane == 0, i_part, jnp.where(lane == 1, f_part, squares))
        high = misc.astype(BF16).astype(F32)
        low = misc - high
        product = jnp.dot(scaled, wcat[c], preferred_element_type=F32)
        blocks = [product[:, 128 * b : 128 * (b + 1)] for b in range(6)] + [high, low]
        for b, block in enumerate(blocks):
            for s in range(2):
                stage[pl.ds(2 * b + s, N, stride=ROWS), :] = block[s * N : (s + 1) * N]
        sbuf[c] = stage[...].reshape(N, ROWS, 128).astype(BF16)
        for o in far_dp:
            send(sbuf.at[c, lax.rem(d + o, N)], rbuf.at[c, N - 1 - o], phase, dp_peer(o))
        sends.append((rbuf.at[c], phase))

    def step_state(c, phase_in, phase_out):
        wait_recv(rbuf.at[c], phase_in)
        acc = sbuf[c, d].astype(F32) + jnp.sum(rbuf[c].astype(F32), axis=0)
        acc_hi = acc.astype(BF16)
        acc_lo = (acc - acc_hi.astype(F32)).astype(BF16)
        read = (
            jnp.dot(acc_hi, cellt_hi[c], preferred_element_type=F32)
            + jnp.dot(acc_lo, cellt_hi[c], preferred_element_type=F32)
            + jnp.dot(acc_hi, cellt_lo[c], preferred_element_type=F32)
        )
        row = lax.broadcasted_iota(jnp.int32, (2, DHV), 0)
        read = jnp.where(row == 0, read[0:2, 0:DHV], read[0:2, DHV : 2 * DHV])
        q0 = acc[0:2]
        k0 = acc[2:4]
        v0 = jnp.concatenate([acc[4:6], acc[6:8]], axis=1)
        o0 = jnp.concatenate([acc[8:10], acc[10:12]], axis=1)
        misc = acc[12:14] + acc[14:16]
        lane = lax.broadcasted_iota(jnp.int32, (2, 128), 1)
        i0 = jnp.sum(jnp.where(lane == 0, misc, 0.0), axis=1, keepdims=True)
        f0 = jnp.sum(jnp.where(lane == 1, misc, 0.0), axis=1, keepdims=True)
        squares = jnp.sum(jnp.where(lane == 2, misc, 0.0), axis=1, keepdims=True)
        kq0 = jnp.sum(k0 * q0, axis=1, keepdims=True)
        nq0 = jnp.sum(norm[c] * q0, axis=1, keepdims=True)
        r = lax.rsqrt(squares / features + EPS)
        rq = r * DHK ** (-0.5)
        i_pre = i0 * r
        f_pre = f0 * r
        pick = lax.broadcasted_iota(jnp.int32, (2, 2), 0) == lax.broadcasted_iota(jnp.int32, (2, 2), 1)
        m = jnp.sum(jnp.where(pick, stab[c], 0.0), axis=1, keepdims=True)
        lf = jnp.minimum(f_pre, 0.0) - jnp.log1p(jnp.exp(-jnp.abs(f_pre)))
        m_next = jnp.maximum(lf + m, i_pre)
        retain = jnp.exp(lf + m - m_next)
        admit = jnp.exp(i_pre - m_next)
        kq = kq0 * r * rq
        den = retain * (nq0 * rq) + admit * kq
        num = (retain * rq) * read + (admit * kq) * (v0 * r)
        gated = num / jnp.maximum(jnp.abs(den), 1.0) * jax.nn.sigmoid(o0 * r)
        gbuf[c, d] = gated.astype(BF16)
        for o in far_dp:
            send(gbuf.at[c, d], gbuf.at[c, d], phase_out, dp_peer(o))
        sends.append((gbuf.at[c, pl.ds(0, N - 1)], phase_out))
        _, c_out, n_out, m_out = None, *outs[1 + 3 * c : 4 + 3 * c]
        k = k0 * r
        n_out[...] = retain * norm[c] + admit * k
        m_out[...] = jnp.sum(jnp.where(pick, m_next, 0.0), axis=0, keepdims=True)
        va = v0 * (r * admit)
        for s in range(2):
            column = jnp.broadcast_to(va[s : s + 1], (8, DHV)).T[:, 0:1]
            cell[c, s * DHV : (s + 1) * DHV, :] = (
                retain[s : s + 1] * cell[c, s * DHV : (s + 1) * DHV, :] + column * k[s : s + 1]
            )
        copy = pltpu.make_async_copy(cell.at[c], c_out, out_sems.at[c])
        copy.start()
        return copy

    def mix(c, phase_in):
        wait_recv(gbuf.at[c, pl.ds(0, N - 1)], phase_in)
        for j in range(N):
            gs[2 * j : 2 * j + 2, :] = gbuf[c, j].astype(F32)
        return jnp.dot(gs[...].astype(BF16), wmix[c], preferred_element_type=F32)

    project(0, 1)
    out_first = step_state(0, 1, 2)
    partial = mix(0, 2)
    ybuf[t] = partial.astype(BF16)
    for o in range(1, T):
        send(ybuf.at[t], ybuf.at[t], 3, tp_peer(o))
    sends.append((ybuf.at[pl.ds(0, T - 1)], 3))
    wait_recv(ybuf.at[pl.ds(0, T - 1)], 3)
    middle = xs[...] + jnp.sum(ybuf[...].astype(F32), axis=0)
    xs[...] = middle.astype(BF16).astype(F32)
    project(1, 4)
    out_second = step_state(1, 4, 5)
    ysc[...] = mix(1, 5)
    for j in range(T):
        ysend[j] = ysc[4 * j : 4 * j + 4, :].astype(BF16)
    for o in range(1, T):
        send(ysend.at[lax.rem(t + o, T)], yrecv.at[T - 1 - o], 6, tp_peer(o))
    sends.append((yrecv, 6))
    own = xs[pl.ds(4 * t, 4), :] + ysc[pl.ds(4 * t, 4), :]
    wait_recv(yrecv, 6)
    outs[0][...] = (own + jnp.sum(yrecv[...].astype(F32), axis=0)).astype(BF16)
    out_first.wait()
    out_second.wait()
    for ref, phase in sends:
        wait_send(ref, phase)


def build(T, N):
    def per_device(*args):
        x = args[0]
        flat = [x]
        for c in range(2):
            gain, wq, wk, wv, wo, wi, wf, wm, state, nstate, mstate = args[1 + 11 * c : 12 + 11 * c]
            flat += [
                gain.reshape(1, DHK),
                wq,
                wk,
                wv,
                wo,
                wi.T,
                wf.T,
                wm,
                state.reshape(2 * DHV, DHK),
                nstate.reshape(2, DHK),
                mstate.T,
            ]
        hbm = pl.BlockSpec(memory_space=pl.ANY)
        vmem = pl.BlockSpec(memory_space=pltpu.VMEM)
        state_shapes = [
            jax.ShapeDtypeStruct((2 * DHV, DHK), F32),
            jax.ShapeDtypeStruct((2, DHK), F32),
            jax.ShapeDtypeStruct((1, 2), F32),
        ]
        B = 4 * T
        got = pl.pallas_call(
            functools.partial(kernel, T, N),
            out_shape=[jax.ShapeDtypeStruct((4, DHK), BF16)] + state_shapes * 2,
            in_specs=[hbm] * len(flat),
            out_specs=[vmem] + [hbm, vmem, vmem] * 2,
            scratch_shapes=[
                pltpu.VMEM((2, DHK, 768), BF16),
                pltpu.VMEM((2, DHV, DHK), BF16),
                pltpu.VMEM((2, 2, T, DHK), BF16),
                pltpu.VMEM((2, 2, 1, DHK), F32),
                pltpu.VMEM((2, 1, DHK), BF16),
                pltpu.VMEM((2, 2 * DHV, DHK), F32),
                pltpu.VMEM((2, 2, DHK), F32),
                pltpu.VMEM((2, 1, 2), F32),
                pltpu.VMEM((2, DHK, 2 * DHV), BF16),
                pltpu.VMEM((2, DHK, 2 * DHV), BF16),
                pltpu.VMEM((T, 4, DHK), BF16),
                pltpu.VMEM((B, DHK), F32),
                pltpu.VMEM((N * ROWS, DHK), F32),
                pltpu.VMEM((2, N, ROWS, DHK), BF16),
                pltpu.VMEM((2, N - 1, ROWS, DHK), BF16),
                pltpu.VMEM((2, N, 2, DHV), BF16),
                pltpu.VMEM((B, DHV), F32),
                pltpu.VMEM((T, B, DHK), BF16),
                pltpu.VMEM((B, DHK), F32),
                pltpu.VMEM((T, 4, DHK), BF16),
                pltpu.VMEM((T - 1, 4, DHK), BF16),
                pltpu.SemaphoreType.DMA((23,)),
                pltpu.SemaphoreType.DMA((2,)),
                pltpu.SemaphoreType.DMA((7,)),
                pltpu.SemaphoreType.DMA((7,)),
            ],
            compiler_params=pltpu.CompilerParams(collective_id=0, has_side_effects=True),
            name="cells",
        )(*flat)
        hidden, c1, n1, m1, c2, n2, m2 = got
        return (
            hidden,
            c1.reshape(2, 1, DHV, DHK),
            n1.reshape(2, 1, DHK),
            m1.T,
            c2.reshape(2, 1, DHV, DHK),
            n2.reshape(2, 1, DHK),
            m2.T,
        )

    return per_device


def solution(mesh):
    cell_specs = (
        P("dp"),
        P("dp", "tp"),
        P("dp", "tp"),
        P("dp", "tp"),
        P("dp", "tp"),
        P("dp", None),
        P("dp", None),
        P("tp", "dp"),
        P("dp", "tp", None, None),
        P("dp", "tp", None),
        P("dp", "tp"),
    )
    state_specs = (P("dp", "tp", None, None), P("dp", "tp", None), P("dp", "tp"))
    return jax.shard_map(
        build(mesh.shape["tp"], mesh.shape["dp"]),
        mesh=mesh,
        in_specs=(P("tp", "dp"),) + cell_specs * 2,
        out_specs=(P("tp", "dp"),) + state_specs * 2,
        check_vma=False,
    )
```

```python
import functools

import jax
import jax.numpy as jnp
from jax import lax
from jax.experimental import pallas as pl
from jax.experimental.pallas import tpu as pltpu
from jax.sharding import PartitionSpec as P

DHK = 128
DHV = 256
EPS = 1e-06
ROWS = 16
MESH = pl.DeviceIdType.MESH
F32 = jnp.float32
BF16 = jnp.bfloat16


def kernel(T, N, *refs):
    (x_in, *rest) = refs
    ins = (rest[:11], rest[11:22])
    outs = rest[22:29]
    (
        wcat,
        wmix,
        wif,
        wif_own,
        gains,
        cell,
        norm,
        stab,
        cellt_hi,
        cellt_lo,
        xg,
        xs,
        stage,
        sbuf,
        rbuf,
        gbuf,
        gs,
        ybuf,
        ysc,
        ysend,
        yrecv,
        load_sems,
        send_sems,
        recv_sems,
    ) = rest[29:]
    t = lax.axis_index("tp")
    d = lax.axis_index("dp")
    features = DHK * N

    def tp_peer(o):
        return {"tp": lax.rem(t + o, T)}

    def dp_peer(o):
        return {"dp": lax.rem(d + o, N)}

    far_dp = sorted(range(1, N), key=lambda o: abs(o - N // 2))

    barrier = pltpu.get_barrier_semaphore()
    for o in far_dp:
        pl.semaphore_signal(barrier, inc=1, device_id=dp_peer(o), device_id_type=MESH)
    for o in range(1, T):
        pl.semaphore_signal(barrier, inc=1, device_id=tp_peer(o), device_id_type=MESH)

    x_load = pltpu.make_async_copy(x_in, xg.at[t], load_sems.at[0])
    x_load.start()
    loads = []
    for c in range(2):
        gain, wq, wk, wv, wo, wi, wf, wm, state, nstate, mstate = ins[c]
        pairs = [
            (gain, gains.at[c]),
            (wq, wcat.at[c, :, 0:128]),
            (wk, wcat.at[c, :, 128:256]),
            (wv, wcat.at[c, :, 256:512]),
            (wo, wcat.at[c, :, 512:768]),
            (wi, wif.at[c, 0]),
            (wf, wif.at[c, 1]),
            (state, cell.at[c]),
            (nstate, norm.at[c]),
            (mstate, stab.at[c]),
            (wm, wmix.at[c]),
        ]
        group = []
        for n, (src, dst) in enumerate(pairs):
            copy = pltpu.make_async_copy(src, dst, load_sems.at[1 + 11 * c + n])
            copy.start()
            group.append(copy)
        loads.append(group)

    def prepare(c):
        mine = lax.broadcasted_iota(jnp.int32, (T, DHK), 0) == t
        for g in range(2):
            wif_own[c, g] = jnp.sum(jnp.where(mine, wif[c, g].astype(F32), 0.0), axis=0, keepdims=True)
        for s in range(2):
            old = cell[c, s * DHV : (s + 1) * DHV, :]
            turned = old.T
            high = turned.astype(BF16)
            cellt_hi[c, :, s * DHV : (s + 1) * DHV] = high
            cellt_lo[c, :, s * DHV : (s + 1) * DHV] = (turned - high.astype(F32)).astype(BF16)

    with jax.named_scope("entry"):
        pl.semaphore_wait(barrier, T + N - 2)

    x_load.wait()
    sends = []

    def send(src, dst, phase, peer):
        copy = pltpu.make_async_remote_copy(
            src_ref=src,
            dst_ref=dst,
            send_sem=send_sems.at[phase],
            recv_sem=recv_sems.at[phase],
            device_id=peer,
            device_id_type=MESH,
        )
        copy.start()
        return copy

    def wait_recv(ref, phase):
        pltpu.make_async_copy(ref, ref, recv_sems.at[phase]).wait()

    def wait_send(ref, phase):
        pltpu.make_async_copy(ref, ref, send_sems.at[phase]).wait()

    for o in range(1, T):
        send(xg.at[t], xg.at[t], 0, tp_peer(o))
    sends.append((xg.at[pl.ds(0, T - 1)], 0))

    for copy in loads[0]:
        copy.wait()
    prepare(0)

    with jax.named_scope("x_wait"):
        wait_recv(xg.at[pl.ds(0, T - 1)], 0)
    for j in range(T):
        xs[4 * j : 4 * j + 4, :] = xg[j].astype(F32)

    def project(c, phase):
        wide = jnp.concatenate([xs[pl.ds(0, N, stride=2), :], xs[pl.ds(1, N, stride=2), :]], axis=0)
        scaled = (wide * gains[c].astype(F32)).astype(BF16)
        squares = jnp.sum(wide * wide, axis=1, keepdims=True)
        scaled_wide = scaled.astype(F32)
        wi_row = wif_own[c, 0]
        wf_row = wif_own[c, 1]
        i_part = jnp.sum(scaled_wide * wi_row, axis=1, keepdims=True)
        f_part = jnp.sum(scaled_wide * wf_row, axis=1, keepdims=True)
        lane = lax.broadcasted_iota(jnp.int32, (2 * N, 128), 1)
        misc = jnp.where(lane == 0, i_part, jnp.where(lane == 1, f_part, squares))
        high = misc.astype(BF16).astype(F32)
        low = misc - high
        product = jnp.dot(scaled, wcat[c], preferred_element_type=F32)
        blocks = [product[:, 128 * b : 128 * (b + 1)] for b in range(6)] + [high, low]
        for b, block in enumerate(blocks):
            for s in range(2):
                stage[pl.ds(2 * b + s, N, stride=ROWS), :] = block[s * N : (s + 1) * N]
        sbuf[c] = stage[...].reshape(N, ROWS, 128).astype(BF16)
        with jax.named_scope("rs_send"):
            for o in far_dp:
                send(sbuf.at[c, lax.rem(d + o, N)], rbuf.at[c, N - 1 - o], phase, dp_peer(o))
        sends.append((rbuf.at[c], phase))

    def step_state(c, phase_in, phase_out):
        with jax.named_scope("rs_wait"):
            wait_recv(rbuf.at[c], phase_in)
        acc = sbuf[c, d].astype(F32) + jnp.sum(rbuf[c].astype(F32), axis=0)
        acc_hi = acc.astype(BF16)
        acc_lo = (acc - acc_hi.astype(F32)).astype(BF16)
        read = (
            jnp.dot(acc_hi, cellt_hi[c], preferred_element_type=F32)
            + jnp.dot(acc_lo, cellt_hi[c], preferred_element_type=F32)
            + jnp.dot(acc_hi, cellt_lo[c], preferred_element_type=F32)
        )
        row = lax.broadcasted_iota(jnp.int32, (2, DHV), 0)
        read = jnp.where(row == 0, read[0:2, 0:DHV], read[0:2, DHV : 2 * DHV])
        q0 = acc[0:2]
        k0 = acc[2:4]
        v0 = jnp.concatenate([acc[4:6], acc[6:8]], axis=1)
        o0 = jnp.concatenate([acc[8:10], acc[10:12]], axis=1)
        misc = acc[12:14] + acc[14:16]
        lane = lax.broadcasted_iota(jnp.int32, (2, 128), 1)
        i0 = jnp.sum(jnp.where(lane == 0, misc, 0.0), axis=1, keepdims=True)
        f0 = jnp.sum(jnp.where(lane == 1, misc, 0.0), axis=1, keepdims=True)
        squares = jnp.sum(jnp.where(lane == 2, misc, 0.0), axis=1, keepdims=True)
        kq0 = jnp.sum(k0 * q0, axis=1, keepdims=True)
        nq0 = jnp.sum(norm[c] * q0, axis=1, keepdims=True)
        r = lax.rsqrt(squares / features + EPS)
        rq = r * DHK ** (-0.5)
        i_pre = i0 * r
        f_pre = f0 * r
        pick = lax.broadcasted_iota(jnp.int32, (2, 2), 0) == lax.broadcasted_iota(jnp.int32, (2, 2), 1)
        m = jnp.sum(jnp.where(pick, stab[c], 0.0), axis=1, keepdims=True)
        lf = jnp.minimum(f_pre, 0.0) - jnp.log1p(jnp.exp(-jnp.abs(f_pre)))
        m_next = jnp.maximum(lf + m, i_pre)
        retain = jnp.exp(lf + m - m_next)
        admit = jnp.exp(i_pre - m_next)
        kq = kq0 * r * rq
        den = retain * (nq0 * rq) + admit * kq
        num = (retain * rq) * read + (admit * kq) * (v0 * r)
        gated = num / jnp.maximum(jnp.abs(den), 1.0) * jax.nn.sigmoid(o0 * r)
        gbuf[c, d] = gated.astype(BF16)
        with jax.named_scope("ag_send"):
            for o in far_dp:
                send(gbuf.at[c, d], gbuf.at[c, d], phase_out, dp_peer(o))
        sends.append((gbuf.at[c, pl.ds(0, N - 1)], phase_out))
        c_out, n_out, m_out = outs[1 + 3 * c : 4 + 3 * c]
        k = k0 * r
        n_out[...] = retain * norm[c] + admit * k
        m_out[...] = jnp.sum(jnp.where(pick, m_next, 0.0), axis=0, keepdims=True)
        va = v0 * (r * admit)
        for s in range(2):
            column = jnp.broadcast_to(va[s : s + 1], (8, DHV)).T[:, 0:1]
            c_out[s * DHV : (s + 1) * DHV, :] = (
                retain[s : s + 1] * cell[c, s * DHV : (s + 1) * DHV, :] + column * k[s : s + 1]
            )

    def mix(c, phase_in):
        with jax.named_scope("ag_wait"):
            wait_recv(gbuf.at[c, pl.ds(0, N - 1)], phase_in)
        for j in range(N):
            gs[2 * j : 2 * j + 2, :] = gbuf[c, j].astype(F32)
        return jnp.dot(gs[...].astype(BF16), wmix[c], preferred_element_type=F32)

    project(0, 1)
    for copy in loads[1]:
        copy.wait()
    prepare(1)
    step_state(0, 1, 2)
    partial = mix(0, 2)
    ybuf[t] = partial.astype(BF16)
    for o in range(1, T):
        send(ybuf.at[t], ybuf.at[t], 3, tp_peer(o))
    sends.append((ybuf.at[pl.ds(0, T - 1)], 3))
    with jax.named_scope("ar_wait"):
        wait_recv(ybuf.at[pl.ds(0, T - 1)], 3)
    middle = xs[...] + jnp.sum(ybuf[...].astype(F32), axis=0)
    xs[...] = middle.astype(BF16).astype(F32)
    project(1, 4)
    step_state(1, 4, 5)
    ysc[...] = mix(1, 5)
    for j in range(T):
        ysend[j] = ysc[4 * j : 4 * j + 4, :].astype(BF16)
    for o in range(1, T):
        send(ysend.at[lax.rem(t + o, T)], yrecv.at[T - 1 - o], 6, tp_peer(o))
    sends.append((yrecv, 6))
    own = xs[pl.ds(4 * t, 4), :] + ysc[pl.ds(4 * t, 4), :]
    with jax.named_scope("y_wait"):
        wait_recv(yrecv, 6)
    outs[0][...] = (own + jnp.sum(yrecv[...].astype(F32), axis=0)).astype(BF16)
    for ref, phase in sends:
        wait_send(ref, phase)


def publish(*refs):
    sems = refs[14]
    copies = [pltpu.make_async_copy(refs[n], refs[7 + n], sems.at[n]) for n in range(7)]
    for copy in copies:
        copy.start()
    for copy in copies:
        copy.wait()


def build(T, N):
    def per_device(*args):
        x = args[0]
        flat = [x]
        for c in range(2):
            gain, wq, wk, wv, wo, wi, wf, wm, state, nstate, mstate = args[1 + 11 * c : 12 + 11 * c]
            flat += [
                gain.reshape(1, DHK),
                wq,
                wk,
                wv,
                wo,
                wi.T,
                wf.T,
                wm,
                state.reshape(2 * DHV, DHK),
                nstate.reshape(2, DHK),
                mstate.T,
            ]
        hbm = pl.BlockSpec(memory_space=pltpu.HBM)
        vmem = pl.BlockSpec(memory_space=pltpu.VMEM)
        state_shapes = [
            ((2 * DHV, DHK), F32),
            ((2, DHK), F32),
            ((1, 2), F32),
        ]
        shapes = [((4, DHK), BF16)] + state_shapes * 2
        B = 4 * T
        got = pl.pallas_call(
            functools.partial(kernel, T, N),
            out_shape=[pltpu.VMEM(*shape) for shape in shapes],
            in_specs=[hbm] * len(flat),
            out_specs=[vmem] * 7,
            scratch_shapes=[
                pltpu.VMEM((2, DHK, 768), BF16),
                pltpu.VMEM((2, DHV, DHK), BF16),
                pltpu.VMEM((2, 2, T, DHK), BF16),
                pltpu.VMEM((2, 2, 1, DHK), F32),
                pltpu.VMEM((2, 1, DHK), BF16),
                pltpu.VMEM((2, 2 * DHV, DHK), F32),
                pltpu.VMEM((2, 2, DHK), F32),
                pltpu.VMEM((2, 1, 2), F32),
                pltpu.VMEM((2, DHK, 2 * DHV), BF16),
                pltpu.VMEM((2, DHK, 2 * DHV), BF16),
                pltpu.VMEM((T, 4, DHK), BF16),
                pltpu.VMEM((B, DHK), F32),
                pltpu.VMEM((N * ROWS, DHK), F32),
                pltpu.VMEM((2, N, ROWS, DHK), BF16),
                pltpu.VMEM((2, N - 1, ROWS, DHK), BF16),
                pltpu.VMEM((2, N, 2, DHV), BF16),
                pltpu.VMEM((B, DHV), F32),
                pltpu.VMEM((T, B, DHK), BF16),
                pltpu.VMEM((B, DHK), F32),
                pltpu.VMEM((T, 4, DHK), BF16),
                pltpu.VMEM((T - 1, 4, DHK), BF16),
                pltpu.SemaphoreType.DMA((23,)),
                pltpu.SemaphoreType.DMA((7,)),
                pltpu.SemaphoreType.DMA((7,)),
            ],
            compiler_params=pltpu.CompilerParams(
                collective_id=0, has_side_effects=True, vmem_limit_bytes=24 * 1024 * 1024
            ),
            name="cells",
        )(*[pltpu.with_memory_space_constraint(a, pltpu.HBM) for a in flat])
        got = pl.pallas_call(
            publish,
            out_shape=[jax.ShapeDtypeStruct(*shape) for shape in shapes],
            in_specs=[vmem] * 7,
            out_specs=[hbm] * 7,
            scratch_shapes=[pltpu.SemaphoreType.DMA((7,))],
            compiler_params=pltpu.CompilerParams(vmem_limit_bytes=1024 * 1024),
            name="publish",
        )(*got)
        hidden, c1, n1, m1, c2, n2, m2 = got
        return (
            hidden,
            c1.reshape(2, 1, DHV, DHK),
            n1.reshape(2, 1, DHK),
            m1.T,
            c2.reshape(2, 1, DHV, DHK),
            n2.reshape(2, 1, DHK),
            m2.T,
        )

    return per_device


def solution(mesh):
    cell_specs = (
        P("dp"),
        P("dp", "tp"),
        P("dp", "tp"),
        P("dp", "tp"),
        P("dp", "tp"),
        P("dp", None),
        P("dp", None),
        P("tp", "dp"),
        P("dp", "tp", None, None),
        P("dp", "tp", None),
        P("dp", "tp"),
    )
    state_specs = (P("dp", "tp", None, None), P("dp", "tp", None), P("dp", "tp"))
    return jax.shard_map(
        build(mesh.shape["tp"], mesh.shape["dp"]),
        mesh=mesh,
        in_specs=(P("tp", "dp"),) + cell_specs * 2,
        out_specs=(P("tp", "dp"),) + state_specs * 2,
        check_vma=False,
    )
```

```python
import functools

import jax
import jax.numpy as jnp
from jax import lax
from jax.experimental import pallas as pl
from jax.experimental.pallas import tpu as pltpu
from jax.sharding import PartitionSpec as P

DHK = 128
DHV = 256
EPS = 1e-06
ROWS = 16
MESH = pl.DeviceIdType.MESH
F32 = jnp.float32
BF16 = jnp.bfloat16


def kernel(T, N, *refs):
    (x_in, *rest) = refs
    ins = (rest[:11], rest[11:22])
    outs = rest[22:29]
    (
        wcat,
        wmix,
        wif,
        wif_own,
        gains,
        cell,
        norm,
        stab,
        cellt_hi,
        cellt_lo,
        xl,
        xg,
        xs,
        xres_send,
        xres,
        stage,
        sbuf,
        rbuf,
        gbuf,
        gs,
        ybuf,
        ysc,
        ysend,
        yrecv,
        load_sems,
        pair_send,
        pair_recv,
        send_sems,
        recv_sems,
    ) = rest[29:]
    t = lax.axis_index("tp")
    d = lax.axis_index("dp")
    Z = N // 2
    c = lax.rem(d, 2)
    z = d // 2
    partner = {"dp": 2 * z + 1 - c}
    features = DHK * N

    TX = 4 if T % 4 == 0 else T
    TY = T // TX
    plane = [(dy, dx) for dy in range(TY) for dx in range(TX)]
    plane.sort(key=lambda o: -(min(o[0], TY - o[0]) + min(o[1], TX - o[1])))
    far_z = sorted(range(1, Z), key=lambda o: abs(o - Z // 2))

    def tp_index(o):
        return lax.rem(t // TX + o[0], TY) * TX + lax.rem(lax.rem(t, TX) + o[1], TX)

    others = [tp_index(o) for o in plane[:-1]]

    def z_peer(o):
        return {"dp": 2 * lax.rem(z + o, Z) + c}

    barrier = pltpu.get_barrier_semaphore()

    def greet(peer):
        pl.semaphore_signal(barrier, inc=1, device_id=peer, device_id_type=MESH)

    for o in far_z:
        greet(z_peer(o))
    for j in others:
        for b in range(2):
            greet({"tp": j, "dp": 2 * z + b})
    greet(partner)

    x_loads = [
        pltpu.make_async_copy(x_in, xl, load_sems.at[0]),
        pltpu.make_async_copy(x_in.at[c], xg.at[2 * t + c], load_sems.at[1]),
    ]
    for copy in x_loads:
        copy.start()
    loads = []
    for n in range(2):
        gain, wq, wk, wv, wo, wi, wf, wm, state, nstate, mstate = ins[n]
        shared = [
            (gain, gains.at[n, c]),
            (wq, wcat.at[n, c, :, 0:128]),
            (wk, wcat.at[n, c, :, 128:256]),
            (wv, wcat.at[n, c, :, 256:512]),
            (wo, wcat.at[n, c, :, 512:768]),
            (wi, wif.at[n, c, 0]),
            (wf, wif.at[n, c, 1]),
            (wm, wmix.at[n, c]),
        ]
        private = [
            (state, cell.at[n]),
            (nstate, norm.at[n]),
            (mstate, stab.at[n]),
        ]
        group = []
        for i, (src, dst) in enumerate(shared + private):
            copy = pltpu.make_async_copy(src, dst, load_sems.at[2 + 11 * n + i])
            copy.start()
            group.append(copy)
        loads.append((shared, group))

    def prepare(n):
        for s in range(2):
            old = cell[n, s * DHV : (s + 1) * DHV, :]
            turned = old.T
            high = turned.astype(BF16)
            cellt_hi[n, :, s * DHV : (s + 1) * DHV] = high
            cellt_lo[n, :, s * DHV : (s + 1) * DHV] = (turned - high.astype(F32)).astype(BF16)

    def own_gates(n):
        mine = lax.broadcasted_iota(jnp.int32, (T, DHK), 0) == t
        for b in range(2):
            for g in range(2):
                wif_own[n, b, g] = jnp.sum(
                    jnp.where(mine, wif[n, b, g].astype(F32), 0.0), axis=0, keepdims=True
                )

    def send(src, dst, phase, peer):
        copy = pltpu.make_async_remote_copy(
            src_ref=src,
            dst_ref=dst,
            send_sem=send_sems.at[phase],
            recv_sem=recv_sems.at[phase],
            device_id=peer,
            device_id_type=MESH,
        )
        copy.start()

    def wait_recv(ref, phase):
        pltpu.make_async_copy(ref, ref, recv_sems.at[phase]).wait()

    def wait_send(ref, phase):
        pltpu.make_async_copy(ref, ref, send_sems.at[phase]).wait()

    sends = []
    pairs = []

    def share(n):
        for i, (src, dst) in enumerate(loads[n][0]):
            copy = pltpu.make_async_remote_copy(
                src_ref=src,
                dst_ref=dst,
                send_sem=pair_send.at[8 * n + i],
                recv_sem=pair_recv.at[8 * n + i],
                device_id=partner,
                device_id_type=MESH,
            )
            copy.start()
            pairs.append(copy)

    def ready(n):
        for copy in loads[n][1]:
            copy.wait()
        for copy in pairs[8 * n : 8 * n + 8]:
            copy.wait_recv()

    for copy in x_loads:
        copy.wait()
    with jax.named_scope("entry"):
        pl.semaphore_wait(barrier, Z - 1 + 2 * T - 1)

    for j in others:
        for b in range(2):
            send(xl.at[b], xg.at[2 * t + c], 0, {"tp": j, "dp": 2 * z + b})
    send(xl.at[1 - c], xg.at[2 * t + c], 0, partner)
    sends.append((xg.at[pl.ds(0, 2 * T - 1)], 0))
    share(0)
    with jax.named_scope("ready"):
        ready(0)
    own_gates(0)
    prepare(0)

    with jax.named_scope("x_wait"):
        wait_recv(xg.at[pl.ds(0, 2 * T - 1)], 0)
    for j in range(T):
        for b in range(2):
            xs[b, 2 * j : 2 * j + 2, :] = xg[2 * j + b].astype(F32)

    def project(n, phase):
        wide = [
            jnp.concatenate(
                [xs[b, pl.ds(0, Z, stride=2), :], xs[b, pl.ds(1, Z, stride=2), :]], axis=0
            )
            for b in range(2)
        ]
        scaled = [(wide[b] * gains[n, b].astype(F32)).astype(BF16) for b in range(2)]
        product = jnp.dot(scaled[0], wcat[n, 0], preferred_element_type=F32) + jnp.dot(
            scaled[1], wcat[n, 1], preferred_element_type=F32
        )
        squares = jnp.sum(wide[0] * wide[0] + wide[1] * wide[1], axis=1, keepdims=True)
        again = [scaled[b].astype(F32) for b in range(2)]
        gate_parts = [
            jnp.sum(
                again[0] * wif_own[n, 0, g] + again[1] * wif_own[n, 1, g], axis=1, keepdims=True
            )
            for g in range(2)
        ]
        lane = lax.broadcasted_iota(jnp.int32, (2 * Z, 128), 1)
        misc = jnp.where(lane == 0, gate_parts[0], jnp.where(lane == 1, gate_parts[1], squares))
        high = misc.astype(BF16).astype(F32)
        low = misc - high
        blocks = [product[:, 128 * b : 128 * (b + 1)] for b in range(6)] + [high, low]
        for b, block in enumerate(blocks):
            for s in range(2):
                stage[pl.ds(2 * b + s, Z, stride=ROWS), :] = block[s * Z : (s + 1) * Z]
        sbuf[n] = stage[...].reshape(Z, ROWS, 128).astype(BF16)
        for o in far_z:
            send(sbuf.at[n, lax.rem(z + o, Z)], rbuf.at[n, Z - 1 - o], phase, z_peer(o))
        sends.append((rbuf.at[n], phase))

    def step_state(n, phase_in, phase_out):
        with jax.named_scope("rs_wait"):
            wait_recv(rbuf.at[n], phase_in)
        acc = sbuf[n, z].astype(F32) + jnp.sum(rbuf[n].astype(F32), axis=0)
        acc_hi = acc.astype(BF16)
        acc_lo = (acc - acc_hi.astype(F32)).astype(BF16)
        read = (
            jnp.dot(acc_hi, cellt_hi[n], preferred_element_type=F32)
            + jnp.dot(acc_lo, cellt_hi[n], preferred_element_type=F32)
            + jnp.dot(acc_hi, cellt_lo[n], preferred_element_type=F32)
        )
        row = lax.broadcasted_iota(jnp.int32, (2, DHV), 0)
        read = jnp.where(row == 0, read[0:2, 0:DHV], read[0:2, DHV : 2 * DHV])
        q0 = acc[0:2]
        k0 = acc[2:4]
        v0 = jnp.concatenate([acc[4:6], acc[6:8]], axis=1)
        o0 = jnp.concatenate([acc[8:10], acc[10:12]], axis=1)
        misc = acc[12:14] + acc[14:16]
        lane = lax.broadcasted_iota(jnp.int32, (2, 128), 1)
        i0 = jnp.sum(jnp.where(lane == 0, misc, 0.0), axis=1, keepdims=True)
        f0 = jnp.sum(jnp.where(lane == 1, misc, 0.0), axis=1, keepdims=True)
        squares = jnp.sum(jnp.where(lane == 2, misc, 0.0), axis=1, keepdims=True)
        kq0 = jnp.sum(k0 * q0, axis=1, keepdims=True)
        nq0 = jnp.sum(norm[n] * q0, axis=1, keepdims=True)
        r = lax.rsqrt(squares / features + EPS)
        rq = r * DHK ** (-0.5)
        i_pre = i0 * r
        f_pre = f0 * r
        pick = lax.broadcasted_iota(jnp.int32, (2, 2), 0) == lax.broadcasted_iota(jnp.int32, (2, 2), 1)
        m = jnp.sum(jnp.where(pick, stab[n], 0.0), axis=1, keepdims=True)
        lf = jnp.minimum(f_pre, 0.0) - jnp.log1p(jnp.exp(-jnp.abs(f_pre)))
        m_next = jnp.maximum(lf + m, i_pre)
        retain = jnp.exp(lf + m - m_next)
        admit = jnp.exp(i_pre - m_next)
        kq = kq0 * r * rq
        den = retain * (nq0 * rq) + admit * kq
        num = (retain * rq) * read + (admit * kq) * (v0 * r)
        gated = num / jnp.maximum(jnp.abs(den), 1.0) * jax.nn.sigmoid(o0 * r)
        gbuf[n, z] = gated.astype(BF16)
        for o in far_z:
            send(gbuf.at[n, z], gbuf.at[n, z], phase_out, z_peer(o))
        sends.append((gbuf.at[n, pl.ds(0, Z - 1)], phase_out))
        c_out, n_out, m_out = outs[1 + 3 * n : 4 + 3 * n]
        k = k0 * r
        n_out[...] = retain * norm[n] + admit * k
        m_out[...] = jnp.sum(jnp.where(pick, m_next, 0.0), axis=0, keepdims=True)
        va = v0 * (r * admit)
        for s in range(2):
            column = jnp.broadcast_to(va[s : s + 1], (8, DHV)).T[:, 0:1]
            c_out[s * DHV : (s + 1) * DHV, :] = (
                retain[s : s + 1] * cell[n, s * DHV : (s + 1) * DHV, :] + column * k[s : s + 1]
            )

    def mix(n, phase_in):
        with jax.named_scope("ag_wait"):
            wait_recv(gbuf.at[n, pl.ds(0, Z - 1)], phase_in)
        for j in range(Z):
            gs[2 * j : 2 * j + 2, :] = gbuf[n, j].astype(F32)
        rows = gs[...].astype(BF16)
        return [jnp.dot(rows, wmix[n, b], preferred_element_type=F32) for b in range(2)]

    project(0, 1)
    share(1)
    with jax.named_scope("ready"):
        ready(1)
    own_gates(1)
    prepare(1)
    step_state(0, 1, 2)
    partial = mix(0, 2)
    for b in range(2):
        ybuf[t, b] = partial[b].astype(BF16)
    for j in others:
        send(ybuf.at[t], ybuf.at[t], 3, {"tp": j})
    sends.append((ybuf.at[pl.ds(0, T - 1)], 3))
    with jax.named_scope("ar_wait"):
        wait_recv(ybuf.at[pl.ds(0, T - 1)], 3)
    for b in range(2):
        middle = xs[b] + jnp.sum(ybuf[:, b].astype(F32), axis=0)
        xs[b] = middle.astype(BF16).astype(F32)
    project(1, 4)
    xres_send[...] = xs[1 - c, pl.ds(2 * t, 2), :].astype(BF16)
    send(xres_send, xres, 6, partner)
    sends.append((xres_send, 6))
    step_state(1, 4, 5)
    last = mix(1, 5)
    for b in range(2):
        ysc[b] = last[b]
    for j in range(T):
        for b in range(2):
            ysend[2 * j + b] = ysc[b, 2 * j : 2 * j + 2, :].astype(BF16)
    for j in others:
        for b in range(2):
            send(ysend.at[2 * j + b], yrecv.at[c * T + t], 7, {"tp": j, "dp": 2 * z + b})
    send(ysend.at[2 * t + 1 - c], yrecv.at[c * T + t], 7, partner)
    sends.append((yrecv.at[pl.ds(0, 2 * T - 1)], 7))
    yrecv[c * T + t] = ysend[2 * t + c]
    wait_recv(xres, 6)
    with jax.named_scope("y_wait"):
        wait_recv(yrecv.at[pl.ds(0, 2 * T - 1)], 7)
    own_x = xs[c, pl.ds(2 * t, 2), :]
    other_x = xres[...].astype(F32)
    for b in range(2):
        stream = jnp.where(c == b, own_x, other_x)
        total = jnp.sum(yrecv[b * T : (b + 1) * T].astype(F32), axis=0)
        outs[0][b] = (stream + total).astype(BF16)
    for ref, phase in sends:
        wait_send(ref, phase)
    for copy in pairs:
        copy.wait_send()


def publish(*refs):
    sems = refs[14]
    copies = [pltpu.make_async_copy(refs[n], refs[7 + n], sems.at[n]) for n in range(7)]
    for copy in copies:
        copy.start()
    for copy in copies:
        copy.wait()


def build(T, N):
    def per_device(*args):
        flat = [args[0].reshape(2, 2, DHK)]
        for n in range(2):
            gain, wq, wk, wv, wo, wi, wf, wm, state, nstate, mstate = args[1 + 11 * n : 12 + 11 * n]
            flat += [
                gain.reshape(1, DHK),
                wq,
                wk,
                wv,
                wo,
                wi.T,
                wf.T,
                wm,
                state.reshape(2 * DHV, DHK),
                nstate.reshape(2, DHK),
                mstate.T,
            ]
        hbm = pl.BlockSpec(memory_space=pltpu.HBM)
        vmem = pl.BlockSpec(memory_space=pltpu.VMEM)
        state_shapes = [
            ((2 * DHV, DHK), F32),
            ((2, DHK), F32),
            ((1, 2), F32),
        ]
        shapes = [((2, 2, DHK), BF16)] + state_shapes * 2
        Z = N // 2
        half = 2 * Z
        got = pl.pallas_call(
            functools.partial(kernel, T, N),
            out_shape=[pltpu.VMEM(*shape) for shape in shapes],
            in_specs=[hbm] * len(flat),
            out_specs=[vmem] * 7,
            scratch_shapes=[
                pltpu.VMEM((2, 2, DHK, 768), BF16),
                pltpu.VMEM((2, 2, DHV, DHK), BF16),
                pltpu.VMEM((2, 2, 2, T, DHK), BF16),
                pltpu.VMEM((2, 2, 2, 1, DHK), F32),
                pltpu.VMEM((2, 2, 1, DHK), BF16),
                pltpu.VMEM((2, 2 * DHV, DHK), F32),
                pltpu.VMEM((2, 2, DHK), F32),
                pltpu.VMEM((2, 1, 2), F32),
                pltpu.VMEM((2, DHK, 2 * DHV), BF16),
                pltpu.VMEM((2, DHK, 2 * DHV), BF16),
                pltpu.VMEM((2, 2, DHK), BF16),
                pltpu.VMEM((2 * T, 2, DHK), BF16),
                pltpu.VMEM((2, half, DHK), F32),
                pltpu.VMEM((2, DHK), BF16),
                pltpu.VMEM((2, DHK), BF16),
                pltpu.VMEM((Z * ROWS, DHK), F32),
                pltpu.VMEM((2, Z, ROWS, DHK), BF16),
                pltpu.VMEM((2, Z - 1, ROWS, DHK), BF16),
                pltpu.VMEM((2, Z, 2, DHV), BF16),
                pltpu.VMEM((half, DHV), F32),
                pltpu.VMEM((T, 2, half, DHK), BF16),
                pltpu.VMEM((2, half, DHK), F32),
                pltpu.VMEM((2 * T, 2, DHK), BF16),
                pltpu.VMEM((2 * T, 2, DHK), BF16),
                pltpu.SemaphoreType.DMA((24,)),
                pltpu.SemaphoreType.DMA((16,)),
                pltpu.SemaphoreType.DMA((16,)),
                pltpu.SemaphoreType.DMA((8,)),
                pltpu.SemaphoreType.DMA((8,)),
            ],
            compiler_params=pltpu.CompilerParams(
                collective_id=0, has_side_effects=True, vmem_limit_bytes=24 * 1024 * 1024
            ),
            name="cells",
        )(*[pltpu.with_memory_space_constraint(a, pltpu.HBM) for a in flat])
        got = pl.pallas_call(
            publish,
            out_shape=[jax.ShapeDtypeStruct(*shape) for shape in shapes],
            in_specs=[vmem] * 7,
            out_specs=[hbm] * 7,
            scratch_shapes=[pltpu.SemaphoreType.DMA((7,))],
            compiler_params=pltpu.CompilerParams(vmem_limit_bytes=1024 * 1024),
            name="publish",
        )(*got)
        hidden, c1, n1, m1, c2, n2, m2 = got
        return (
            hidden.reshape(4, DHK),
            c1.reshape(2, 1, DHV, DHK),
            n1.reshape(2, 1, DHK),
            m1.T,
            c2.reshape(2, 1, DHV, DHK),
            n2.reshape(2, 1, DHK),
            m2.T,
        )

    return per_device


def solution(mesh):
    cell_specs = (
        P("dp"),
        P("dp", "tp"),
        P("dp", "tp"),
        P("dp", "tp"),
        P("dp", "tp"),
        P("dp", None),
        P("dp", None),
        P("tp", "dp"),
        P("dp", "tp", None, None),
        P("dp", "tp", None),
        P("dp", "tp"),
    )
    state_specs = (P("dp", "tp", None, None), P("dp", "tp", None), P("dp", "tp"))
    return jax.shard_map(
        build(mesh.shape["tp"], mesh.shape["dp"]),
        mesh=mesh,
        in_specs=(P("tp", "dp"),) + cell_specs * 2,
        out_specs=(P("tp", "dp"),) + state_specs * 2,
        check_vma=False,
    )
```
